32 devices in a mesh: sp: 8 (over z, x), tp: 4 (over y, core).
Axes of the slice: x: 2, y: 2, z: 4, core: 2. Of those that a mesh axis runs over, the one named last changes fastest.
Arguments:
- hidden_in: bfloat16 [3072, 2048], P('sp', 'tp'), may hold values from -6 to 6
- in_gain: float32 [2048], replicated, may hold values from 0.1 to 1.9
- receptance_weight: bfloat16 [2048, 1024], P(None, 'tp'), may hold values from -0.125 to 0.125
- key_weight: bfloat16 [2048, 1024], P(None, 'tp'), may hold values from -0.125 to 0.125
- value_weight: bfloat16 [2048, 1024], P(None, 'tp'), may hold values from -0.125 to 0.125
- decay_down: bfloat16 [2048, 128], replicated, may hold values from -0.125 to 0.125
- decay_up: bfloat16 [128, 1024], P(None, 'tp'), may hold values from -0.5 to 0.5
- decay_base: float32 [1024], P('tp'), may hold values from -14 to -2
- decay_shift: float32 [3072, 1024], P('sp', 'tp'), may hold values from -1 to 0
- learn_rate: float32 [1024], P('tp'), may hold values from 0 to 1
- query_pair: bfloat16 [2048, 8, 128], P(None, 'tp'), may hold values from -1 to 1
- key_pair: bfloat16 [2048, 8, 128], P(None, 'tp'), may hold values from -1 to 1
- value_pair: bfloat16 [2048, 8, 128], P(None, 'tp'), may hold values from -0.125 to 0.125
- mix_lambda: float32 [8], P('tp'), may hold values from 0.3 to 0.8
- out_recurrent: bfloat16 [1024, 2048], P('tp'), may hold values from -0.1875 to 0.1875
- out_attention: bfloat16 [1024, 2048], P('tp'), may hold values from -0.1875 to 0.1875
- out_gain: float32 [2048], replicated, may hold values from 0.1 to 1.9
Outputs:
- layer_out: bfloat16 [3072, 2048], P(('sp', 'tp'))
- log_sums: float32 [8, 2, 3072], P('tp', None, 'sp')
The draws below stay inside these ranges and needn't reach their ends.
All inputs are finite; a program needn't handle non-finite values.
Results may differ from the reference program's by a relative error of at most 0.018.
Values may be sent and summed in bfloat16 or wider, within the bound.
A program may use at most 128 MiB of HBM per device.

```python
import math
import jax
import jax.numpy as jnp
from jax import lax

D = 2048
RH = 16
DH = 8
HD = 64
LOW = 128
TOK_DEV = 384
TOKENS = 3072
RD = 1024
DW = 1024


def paired_maps(key):
    base = jax.random.fold_in(key, 101)
    leading = jax.random.normal(jax.random.fold_in(base, 1), (D, DH, 2 * HD), jnp.float32) * (3.0 / D) ** 0.5
    trailing = jax.random.normal(jax.random.fold_in(base, 2), (D, DH, 2 * HD), jnp.float32) * D ** (-0.5)
    return (jnp.clip(leading, -1.0, 1.0), jnp.clip(trailing, -1.0, 1.0))


def draw_query_pair(key, part):
    return paired_maps(key)[0].astype(jnp.bfloat16)


def draw_key_pair(key, part):
    return paired_maps(key)[1].astype(jnp.bfloat16)


def draw_hidden_in(key, part):
    rows = jax.random.normal(jax.random.fold_in(key, 7), (TOKENS, D), jnp.float32)
    return jnp.clip(rows, -6.0, 6.0).astype(jnp.bfloat16)


def draw_decay_base(key, part):
    base = jax.random.fold_in(key, 23)
    share = 0.5
    slow = jax.random.uniform(jax.random.fold_in(base, 1), (RH, 1), jnp.float32) < share
    slow_level = jnp.log(jax.random.uniform(jax.random.fold_in(base, 2), (RH, HD), jnp.float32, 0.05, 0.25) / TOKENS)
    fast_level = jax.random.uniform(jax.random.fold_in(base, 3), (RH, HD), jnp.float32, -3.5, -2.0)
    return jnp.where(slow, slow_level, fast_level).reshape(RH * HD)


def draw_decay_shift(key, part):
    base = jax.random.fold_in(key, 31)
    block_total = TOKENS // TOK_DEV
    rates = jnp.exp(jax.random.uniform(jax.random.fold_in(base, 1), (block_total, 1, 1), jnp.float32, math.log(0.1), math.log(0.4))) / TOKENS
    steady = jnp.broadcast_to(rates, (block_total, TOK_DEV, RH * HD)).reshape(TOKENS, RH * HD)
    places = jax.random.randint(jax.random.fold_in(base, 2), (3,), 0, TOKENS)
    sizes = jax.random.uniform(jax.random.fold_in(base, 3), (3, RH * HD), jnp.float32, 0.22, 0.3)
    hits = (jnp.arange(TOKENS)[:, None] == places[None, :]).astype(jnp.float32)
    return -(steady + jnp.dot(hits, sizes))


def draw_learn_rate(key, part):
    base = jax.random.fold_in(key, 41)
    weak_level = jax.random.uniform(jax.random.fold_in(base, 1), (RH * HD,), jnp.float32, math.log(4.0), math.log(40.0))
    weak = jnp.exp(weak_level) / TOKENS
    strong = jnp.exp(jax.random.uniform(jax.random.fold_in(base, 2), (RH * HD,), jnp.float32, math.log(0.05), math.log(0.8)))
    picked = jax.random.randint(jax.random.fold_in(base, 3), (RH * HD,), 0, 8) < 5
    return jnp.where(picked, strong, weak)


def block_levels(rng, dims, shards, smallest, top_value):
    def one(position, blocks):
        heights = jax.random.uniform(jax.random.fold_in(jax.random.fold_in(rng, 6), position), (blocks,), jnp.float32, smallest / len(shards), top_value / len(shards))
        return jnp.repeat(jnp.exp(heights), dims[position] // blocks).reshape((-1,) + (1,) * (len(dims) - position - 1))

    level = one(*shards[0])
    for cut in shards[1:]:
        level = level * one(*cut)
    return level


def bell_draw(key, dims, scale, reach, pieces=(), held_as=jnp.bfloat16):
    values = scale * jax.random.normal(key, dims, jnp.float32)
    if pieces:
        values = values * block_levels(key, dims, pieces, -0.22, 0.18)
    return jnp.clip(values, -reach, reach).astype(held_as)


def setup_inputs(seed: int = 0) -> dict:
    key_list = jax.random.split(jax.random.key(seed), 18)
    return {
        "hidden_in": draw_hidden_in(jax.random.fold_in(key_list[17], 71), 0),
        "in_gain": jnp.clip(1.0 + 0.18 * jax.random.normal(key_list[1], (D,), jnp.float32), 0.1, 1.9),
        "receptance_weight": bell_draw(key_list[2], (D, RD), D ** -0.5, 0.125, ((1, 4),)),
        "key_weight": bell_draw(key_list[3], (D, RD), D ** -0.5, 0.125, ((1, 4),)),
        "value_weight": bell_draw(key_list[4], (D, RD), D ** -0.5, 0.125, ((1, 4),)),
        "decay_down": bell_draw(key_list[5], (D, LOW), D ** -0.5, 0.125),
        "decay_up": bell_draw(key_list[6], (LOW, RD), LOW ** -0.5, 0.5, ((1, 4),)),
        "decay_base": draw_decay_base(jax.random.fold_in(key_list[17], 71), 0),
        "decay_shift": draw_decay_shift(jax.random.fold_in(key_list[17], 71), 0),
        "learn_rate": draw_learn_rate(jax.random.fold_in(key_list[17], 71), 0),
        "query_pair": draw_query_pair(jax.random.fold_in(key_list[17], 71), 0),
        "key_pair": draw_key_pair(jax.random.fold_in(key_list[17], 71), 0),
        "value_pair": bell_draw(key_list[12], (D, DH, 2 * HD), D ** -0.5, 0.125, ((1, 4),)),
        "mix_lambda": jnp.clip(0.3 + 0.5 * jax.random.uniform(key_list[13], (DH,), jnp.float32) ** block_levels(key_list[13], (DH,), ((0, 4),), -0.2, 0.2), 0.3, 0.8),
        "out_recurrent": bell_draw(key_list[14], (RD, D), RD ** -0.5, 0.1875, ((0, 4),)),
        "out_attention": bell_draw(key_list[15], (DW, D), DW ** -0.5, 0.1875, ((0, 4),)),
        "out_gain": jnp.clip(1.0 + 0.18 * jax.random.normal(key_list[16], (D,), jnp.float32), 0.1, 1.9),
    }


HIGHEST = lax.Precision.HIGHEST
DECAY_SCALE = math.exp(-0.5)
NORM_EPS = 1e-06
GROUP_EPS = 0.00064
HEAD_EPS = 1e-05
KEY_EPS = 1e-06

def rms_rows(values, gain):
    wide = values.astype(jnp.float32)
    return wide * lax.rsqrt(lax.optimization_barrier(jnp.mean(wide * wide, axis=-1, keepdims=True)) + NORM_EPS) * gain

def project(normed, weight):
    return jnp.dot(normed, weight.reshape(D, -1), preferred_element_type=jnp.float32).astype(jnp.bfloat16)

def recurrence(receptance, key_rows, value_rows, log_decay, learn_rate):
    shape = (TOKENS, RH, HD)
    receptance = receptance.astype(jnp.float32).reshape(shape)
    key_rows = key_rows.astype(jnp.float32).reshape(shape)
    value_rows = value_rows.astype(jnp.float32).reshape(shape)
    decay = jnp.exp(log_decay).reshape(shape)
    unit_keys = key_rows * lax.rsqrt(lax.optimization_barrier(jnp.sum(key_rows * key_rows, axis=-1, keepdims=True)) + KEY_EPS)
    erasing = unit_keys * learn_rate.reshape(RH, HD)

    def advance(carried, inputs):
        read_now, decay_now, key_now, value_now, unit_now, erase_now = inputs
        removed = jnp.einsum('hvk,hk->hv', carried, unit_now, precision=HIGHEST)
        carried = carried * decay_now[:, None, :] - removed[:, :, None] * erase_now[:, None, :] + value_now[:, :, None] * key_now[:, None, :]
        return (carried, jnp.einsum('hvk,hk->hv', carried, read_now, precision=HIGHEST))
    initial = jnp.zeros((RH, HD, HD), jnp.float32)
    outputs = lax.scan(advance, initial, (receptance, decay, key_rows, value_rows, unit_keys, erasing))[1]
    centered = outputs - lax.optimization_barrier(jnp.mean(outputs, axis=-1, keepdims=True))
    normal = centered * lax.rsqrt(lax.optimization_barrier(jnp.mean(centered * centered, axis=-1, keepdims=True)) + GROUP_EPS)
    return normal.reshape(TOKENS, RH * HD).astype(jnp.bfloat16)

def differential(queries, pair_keys, pair_values, mix_lambda):
    places = jnp.arange(TOKENS)
    score_scale = HD ** (-0.5)
    block_count = TOKENS // TOK_DEV

    def one_head(inputs):
        head_queries, head_keys, head_values, head_lambda = inputs
        keys_wide = head_keys.astype(jnp.float32).reshape(TOKENS, 2, HD)
        values_wide = head_values.astype(jnp.float32)
        query_blocks = head_queries.reshape(block_count, TOK_DEV, 2, HD)

        def one_block(block_inputs):
            block_queries, block_number = block_inputs
            rows_at = block_number * TOK_DEV + jnp.arange(TOK_DEV)
            scores = jnp.einsum('qmd,kmd->mqk', block_queries.astype(jnp.float32), keys_wide) * score_scale
            allowed = rows_at[:, None] >= places[None, :]
            scores = jnp.where(allowed[None], scores, -jnp.inf)
            row_max = lax.optimization_barrier(jnp.max(scores, axis=-1, keepdims=True))
            weights = jnp.exp(scores - row_max)
            row_sum = lax.optimization_barrier(jnp.sum(weights, axis=-1, keepdims=True))
            rounded = lax.optimization_barrier(weights.astype(jnp.bfloat16)).astype(jnp.float32)
            map_out = jnp.einsum('mqk,kv->mqv', rounded, values_wide) / row_sum
            head_out = map_out[0] - head_lambda * map_out[1]
            head_out = head_out * lax.rsqrt(lax.optimization_barrier(jnp.mean(head_out * head_out, axis=-1, keepdims=True)) + HEAD_EPS)
            return (head_out, (row_max + jnp.log(row_sum))[..., 0])
        outs, sums = lax.map(one_block, (query_blocks, jnp.arange(block_count)))
        return (outs.reshape(TOKENS, 2 * HD), sums.transpose(1, 0, 2).reshape(2, TOKENS))
    head_outs, log_sums = lax.map(one_head, (queries.transpose(1, 0, 2), pair_keys.transpose(1, 0, 2), pair_values.transpose(1, 0, 2), mix_lambda))
    att_mix = head_outs.transpose(1, 0, 2).reshape(TOKENS, DH * 2 * HD).astype(jnp.bfloat16)
    return (att_mix, log_sums)

def reference(hidden_in, in_gain, receptance_weight, key_weight, value_weight, decay_down, decay_up, decay_base, decay_shift, learn_rate, query_pair, key_pair, value_pair, mix_lambda, out_recurrent, out_attention, out_gain):
    normed = rms_rows(hidden_in, in_gain).astype(jnp.bfloat16)
    receptance = project(normed, receptance_weight)
    rec_keys = project(normed, key_weight)
    rec_values = project(normed, value_weight)
    low_rank = jnp.tanh(jnp.dot(normed, decay_down, preferred_element_type=jnp.float32)).astype(jnp.bfloat16)
    log_decay = -DECAY_SCALE * jax.nn.sigmoid(jnp.dot(low_rank, decay_up, preferred_element_type=jnp.float32) + decay_base) + decay_shift
    rec_mix = recurrence(receptance, rec_keys, rec_values, log_decay, learn_rate)
    queries = project(normed, query_pair).reshape(TOKENS, DH, 2 * HD)
    pair_keys = project(normed, key_pair).reshape(TOKENS, DH, 2 * HD)
    pair_values = project(normed, value_pair).reshape(TOKENS, DH, 2 * HD)
    att_mix, log_sums = differential(queries, pair_keys, pair_values, mix_lambda)
    projected = jnp.dot(rec_mix, out_recurrent, preferred_element_type=jnp.float32) + jnp.dot(att_mix, out_attention, preferred_element_type=jnp.float32)
    return (rms_rows(projected, out_gain).astype(jnp.bfloat16), log_sums)
```

```python
import functools
import math

import jax
import jax.numpy as jnp
from jax import lax
from jax.experimental import pallas as pl
from jax.experimental.pallas import tpu as pltpu
from jax.sharding import PartitionSpec as P

HD = 64
LANES = 128
CHUNK = 64
DECAY_SCALE = math.exp(-0.5)
NORM_EPS = 1e-06
GROUP_EPS = 0.00064
HEAD_EPS = 1e-05
KEY_EPS = 1e-06
NEGATIVE = -1e30
F32 = jnp.float32
BF16 = jnp.bfloat16


NN = (((1,), (0,)), ((), ()))
NT = (((1,), (1,)), ((), ()))
TN = (((0,), (0,)), ((), ()))


def dot1(a, b, dims=NN):
    return lax.dot_general(a.astype(BF16), b.astype(BF16), dims, preferred_element_type=F32)


def halves(a):
    high = a.astype(BF16)
    return high, (a - high.astype(F32)).astype(BF16)


def dot3(a, b, dims=NN):
    ah, al = halves(a)
    bh, bl = halves(b)
    one = functools.partial(lax.dot_general, dimension_numbers=dims, preferred_element_type=F32)
    return one(ah, bh) + (one(al, bh) + one(ah, bl))


def vmem(count):
    return [pl.BlockSpec(memory_space=pltpu.VMEM)] * count


def call(body, outs, args, scratch=(), flops=1e9):
    return pl.pallas_call(
        body,
        out_shape=outs,
        in_specs=vmem(len(args)),
        out_specs=vmem(len(outs)),
        scratch_shapes=scratch,
        compiler_params=pltpu.CompilerParams(vmem_limit_bytes=56 * 1024 * 1024),
        cost_estimate=pl.CostEstimate(
            flops=int(flops), bytes_accessed=8_000_000, transcendentals=0
        ),
    )(*args)


def project_body(count, *refs):
    pieces = refs[:count]
    gain, wr, wk, wv, down, up, base, shift, wq, wkp, wvp = refs[count : count + 11]
    r_out, k_out, v_out, d_out, q_out, kv_out, normed = refs[count + 11 :]
    me = lax.axis_index("tp")
    width = pieces[0].shape[1]
    wides = [piece[...].astype(F32) for piece in pieces]
    total = sum(jnp.sum(wide * wide, axis=-1, keepdims=True) for wide in wides)
    scale = lax.rsqrt(total / (width * count) + NORM_EPS)
    for turn, wide in enumerate(wides):
        columns = pl.ds(pl.multiple_of((me ^ turn) * width, LANES), width)
        normed[:, columns] = (wide * scale * gain[:, columns]).astype(BF16)

    def product(weight):
        return jnp.dot(normed[...], weight[...], preferred_element_type=F32)

    features = wkp.shape[1]
    kv_out[:, :features] = product(wkp).astype(BF16)
    kv_out[:, features:] = product(wvp).astype(BF16)
    q_out[...] = product(wq).astype(BF16)
    r_out[...] = product(wr).astype(BF16)
    k_out[...] = product(wk).astype(BF16)
    v_out[...] = product(wv).astype(BF16)
    low_rank = jnp.tanh(product(down)).astype(BF16)
    pre = jnp.dot(low_rank, up[...], preferred_element_type=F32) + base[...]
    d_out[...] = -DECAY_SCALE * jax.nn.sigmoid(pre) + shift[...]


def recurrent_body(group, r_ref, k_ref, v_ref, d_ref, learn_ref, out_ref, turn_ref, end_ref, state):
    rows, features = r_ref.shape
    pairs = features // LANES
    lane = lax.broadcasted_iota(jnp.int32, (1, LANES), 1)
    first = (lane < HD).astype(F32)
    second = 1.0 - first
    line = lax.broadcasted_iota(jnp.int32, (LANES, LANES), 0)
    column = lax.broadcasted_iota(jnp.int32, (LANES, LANES), 1)
    strict = line > column
    causal = line >= column
    eye = (line == column).astype(F32)
    same_head = ((line // HD) == (column // HD)).astype(BF16)
    small_line = lax.broadcasted_iota(jnp.int32, (CHUNK, CHUNK), 0)
    small_column = lax.broadcasted_iota(jnp.int32, (CHUNK, CHUNK), 1)
    lower = (small_line >= small_column).astype(BF16)

    def below(size):
        return ((line // size) == (column // size) + 1) & ((line // size) % 2 == 1)

    def spread(x):
        return jnp.concatenate([x * first, x * second], axis=0)

    for pair in range(pairs):
        state[pair, :LANES, :] = jnp.zeros((LANES, LANES), F32)
        state[pair, LANES:, :] = eye

    def local(pair, at):
        here = (pl.ds(at, CHUNK), pl.ds(pair * LANES, LANES))
        r = r_ref[here].astype(F32)
        k = k_ref[here].astype(F32)
        v = v_ref[here].astype(F32)
        decay = d_ref[here]
        learn = learn_ref[:, pl.ds(pair * LANES, LANES)]
        dh = decay.astype(BF16)
        rest = decay - dh.astype(F32)
        dm = rest.astype(BF16)
        dl = (rest - dm.astype(F32)).astype(BF16)
        running = dot1(lower, dh) + (dot1(lower, dm) + dot1(lower, dl))
        before = running - decay
        middle = running[CHUNK // 2 - 1 : CHUNK // 2, :]
        ending = running[CHUNK - 1 :, :]
        sh, sl = halves(k * k)
        squares = dot1(sh, same_head) + dot1(sl, same_head)
        unit = k * lax.rsqrt(squares + KEY_EPS)
        erase = unit * learn
        rise = jnp.exp(middle - running)
        left = jnp.concatenate(
            [spread(-unit * jnp.exp(before - middle)), spread(r * jnp.exp(running - middle))], axis=0
        )
        right = jnp.concatenate([spread(erase * rise), spread(k * rise)], axis=0)
        to_end = jnp.exp(ending - running)
        return dict(
            left=left,
            right=right,
            against=spread(-unit * jnp.exp(before)),
            read=spread(r * jnp.exp(running)),
            erase_end=spread(erase * to_end),
            keys_end=spread(k * to_end),
            values=spread(v),
            whole=jnp.exp(ending),
        )

    def step(turn, carry):
        spots = [(turn * group + g, pair) for g in range(group) for pair in range(pairs)]
        items = [local(pair, pl.multiple_of(c * CHUNK, CHUNK)) for c, pair in spots]
        for it in items:
            scores = dot3(it["left"], it["right"], NT)
            it["low"] = jnp.where(strict, scores[:LANES, :LANES], 0.0)
            it["carry"] = jnp.where(strict, scores[:LANES, LANES:], 0.0)
            it["read_erase"] = jnp.where(causal, scores[LANES:, :LANES], 0.0)
            it["read_keys"] = jnp.where(causal, scores[LANES:, LANES:], 0.0)
            it["inv"] = eye + jnp.where(below(1), it["low"], 0.0)
        size = 2
        while size < CHUNK:
            keep = below(size)
            for it in items:
                it["mid"] = dot3(jnp.where(keep, it["low"], 0.0), it["inv"])
            for it in items:
                it["inv"] = it["inv"] + dot3(it["inv"], it["mid"])
            size *= 2
        for it in items:
            it["fed"] = dot3(it["carry"], it["values"])
        for it in items:
            side = jnp.concatenate([it["against"], it["fed"]], axis=1)
            it["solved"] = dot3(it["inv"], side)
        for it in items:
            seen = dot1(it["read_erase"], it["solved"])
            it["heard"] = seen[:, LANES:] + dot1(it["read_keys"], it["values"])
            it["read"] = it["read"] + seen[:, :LANES]
            it["added"] = dot3(it["values"], it["keys_end"], TN)
        for (c, pair), it in zip(spots, items):
            now = state[pair]
            both = jnp.concatenate([it["solved"][:, :LANES], it["read"]], axis=0)
            met = dot3(both, now, NT)
            gone = jnp.concatenate(
                [met[:LANES, :LANES] + it["solved"][:, LANES:], met[:LANES, LANES:]], axis=1
            )
            later = now * it["whole"] + dot3(gone, it["erase_end"], TN)
            state[pair, :LANES, :] = later[:LANES] + it["added"]
            state[pair, LANES:, :] = later[LANES:]
            heard = met[LANES:, :LANES] + it["heard"]
            turned = met[LANES:, LANES:]
            here = (pl.ds(pl.multiple_of(c * CHUNK, CHUNK), CHUNK), pl.ds(pair * LANES, LANES))
            out_ref[here] = heard[:CHUNK] + heard[CHUNK:]
            turn_ref[here] = turned[:CHUNK] + turned[CHUNK:]
        return carry

    lax.fori_loop(0, rows // CHUNK // group, step, 0)
    for pair in range(pairs):
        now = state[pair]
        end_ref[pair, :HD, :] = (now[:HD] + now[HD:LANES]).astype(BF16)
        end_ref[pair, HD:, :] = (now[LANES : LANES + HD] + now[LANES + HD :]).astype(BF16)


def finish_body(count, *refs):
    out_ref, turn_ref = refs[:2]
    ends = refs[2 : 2 + count]
    mix_ref = refs[2 + count]
    pairs = ends[0].shape[0]
    lane = lax.broadcasted_iota(jnp.int32, (1, LANES), 1)
    first = (lane < HD).astype(F32)
    second = 1.0 - first
    line = lax.broadcasted_iota(jnp.int32, (LANES, LANES), 0)
    column = lax.broadcasted_iota(jnp.int32, (LANES, LANES), 1)
    same_head = ((line // HD) == (column // HD)).astype(BF16)

    def spread(x):
        return jnp.concatenate([x * first, x * second], axis=0)

    for pair in range(pairs):
        entering = jnp.zeros((LANES, LANES), F32)
        for end in ends:
            block = end[pair].astype(F32)
            high, low = halves(entering)
            move = spread(block[HD:])
            entering = dot1(high, move) + dot1(low, move) + spread(block[:HD])
        columns = pl.ds(pair * LANES, LANES)
        full = out_ref[:, columns] + dot3(turn_ref[:, columns], entering, NT)

        def mean(x):
            high, low = halves(x)
            return (dot1(high, same_head) + dot1(low, same_head)) * (1.0 / HD)

        centered = full - mean(full)
        mix_ref[:, columns] = (centered * lax.rsqrt(mean(centered * centered) + GROUP_EPS)).astype(
            BF16
        )


def attend(q, blocks, valid, heads, head, at, tile, diagonal, earlier):
    lane = lax.broadcasted_iota(jnp.int32, (1, LANES), 1)
    part = q[pl.ds(at, tile), pl.ds(head * LANES, LANES)].astype(F32) * HD ** (-0.5)
    both = jnp.concatenate(
        [jnp.where(lane < HD, part, 0.0), jnp.where(lane < HD, 0.0, part)], axis=0
    ).astype(BF16)
    scores = []
    for number, (block, fine) in enumerate(zip(blocks, valid)):
        s = lax.dot_general(
            both, block[:, pl.ds(head * LANES, LANES)], NT, preferred_element_type=F32
        )
        if number == 0 and diagonal:
            line = lax.broadcasted_iota(jnp.int32, (tile, s.shape[1]), 0) + at
            seen = line >= lax.broadcasted_iota(jnp.int32, (tile, s.shape[1]), 1)
            s = jnp.where(jnp.concatenate([seen, seen], axis=0), s, NEGATIVE)
        else:
            s = jnp.where(fine, s, NEGATIVE)
        scores.append(s)
    top = functools.reduce(jnp.maximum, [jnp.max(s, axis=-1, keepdims=True) for s in scores])
    if earlier is not None:
        top = jnp.maximum(top, earlier[0])
    row_sum, acc = 0.0, 0.0
    for s, block in zip(scores, blocks):
        weights = jnp.exp(s - top)
        row_sum = row_sum + jnp.sum(weights, axis=-1, keepdims=True)
        acc = acc + jnp.dot(
            weights.astype(BF16),
            block[:, pl.ds((heads + head) * LANES, LANES)],
            preferred_element_type=F32,
        )
    if earlier is not None:
        fade = jnp.exp(earlier[0] - top)
        row_sum = row_sum + earlier[1] * fade
        acc = acc + earlier[2] * fade
    return top, row_sum, acc


def tiles_of(rows):
    tile = LANES if rows % LANES == 0 else rows
    return tile, range(0, rows, tile)


def near_body(count, q, *refs):
    blocks = refs[:count]
    top_ref, sum_ref, acc_ref = refs[count:]
    rows, features = q.shape
    heads = features // LANES
    place = lax.axis_index("sp")
    tile, starts = tiles_of(rows)
    valid = [place >= 2 * turn for turn in range(count)]
    for head in range(heads):
        for at in starts:
            top, row_sum, acc = attend(q, blocks, valid, heads, head, at, tile, True, None)
            here = pl.ds(2 * at, 2 * tile)
            top_ref[head, here, :] = top
            sum_ref[head, here, :] = row_sum
            acc_ref[head, here, :] = acc


def far_body(count, q, lam_ref, *refs):
    blocks = refs[:count]
    top_ref, sum_ref, acc_ref, mix_ref, log_ref = refs[count:]
    rows, features = q.shape
    heads = features // LANES
    place = lax.axis_index("sp")
    other = place ^ 1
    tile, starts = tiles_of(rows)
    valid = [(other >= 2 * turn) & (other - 2 * turn < place) for turn in range(count)]
    for head in range(heads):
        lam = lam_ref[head]
        for at in starts:
            here = pl.ds(2 * at, 2 * tile)
            earlier = (top_ref[head, here, :], sum_ref[head, here, :], acc_ref[head, here, :])
            top, row_sum, acc = attend(q, blocks, valid, heads, head, at, tile, False, earlier)
            maps = acc / row_sum
            logs = top + jnp.log(row_sum)
            log_ref[head, 0, pl.ds(at, tile), :] = logs[:tile]
            log_ref[head, 1, pl.ds(at, tile), :] = logs[tile:]
            out = maps[:tile] - lam * maps[tile:]
            out = out * lax.rsqrt(jnp.mean(out * out, axis=-1, keepdims=True) + HEAD_EPS)
            mix_ref[pl.ds(at, tile), pl.ds(head * LANES, LANES)] = out.astype(BF16)


def output_body(count, *refs):
    pieces = refs[:count]
    recs = refs[count : 2 * count]
    atts = refs[2 * count : 3 * count]
    gain, out = refs[3 * count :]
    depth = recs[0].shape[0]
    total = 0.0
    for piece, rec, att in zip(pieces, recs, atts):
        total = total + jnp.dot(piece[:, :depth], rec[...], preferred_element_type=F32)
        total = total + jnp.dot(piece[:, depth:], att[...], preferred_element_type=F32)
    mean = jnp.mean(total * total, axis=-1, keepdims=True)
    out[...] = (total * lax.rsqrt(mean + NORM_EPS) * gain[...]).astype(BF16)


def flip(x, axis, size, bit):
    return lax.ppermute(x, axis, [(i, i ^ bit) for i in range(size)])


def gather_pieces(x, size):
    pieces = [x]
    bit = size // 2
    held = {0: x}
    while bit >= 1:
        for turn in list(held):
            held[turn ^ bit] = flip(held[turn], "tp", size, bit)
        bit //= 2
    pieces = [held[turn] for turn in range(size)]
    return pieces


def per_device(
    sp,
    tp,
    hidden_in,
    in_gain,
    receptance_weight,
    key_weight,
    value_weight,
    decay_down,
    decay_up,
    decay_base,
    decay_shift,
    learn_rate,
    query_pair,
    key_pair,
    value_pair,
    mix_lambda,
    out_recurrent,
    out_attention,
    out_gain,
):
    rows = hidden_in.shape[0]
    features = receptance_weight.shape[1]
    heads = mix_lambda.shape[0]
    wide = heads * LANES
    depth = hidden_in.shape[1] * tp
    pairs = features // LANES
    shape = jax.ShapeDtypeStruct

    pieces = gather_pieces(hidden_in, tp)
    r, k, v, log_decay, queries, kv = call(
        functools.partial(project_body, tp),
        [shape((rows, features), BF16)] * 3
        + [shape((rows, features), F32), shape((rows, wide), BF16), shape((rows, 2 * wide), BF16)],
        (
            *pieces,
            in_gain.reshape(1, -1),
            receptance_weight,
            key_weight,
            value_weight,
            decay_down,
            decay_up,
            decay_base.reshape(1, -1),
            decay_shift,
            query_pair.reshape(depth, wide),
            key_pair.reshape(depth, wide),
            value_pair.reshape(depth, wide),
        ),
        [pltpu.VMEM((rows, depth), BF16)],
        flops=3e9,
    )
    near = [kv] + [
        lax.ppermute(kv, "sp", [(i, i + d) for i in range(sp - d)]) for d in range(2, sp, 2)
    ]
    out_recurrent, out_attention, pin = lax.optimization_barrier((out_recurrent, out_attention, kv))
    recs = gather_pieces(out_recurrent, tp)
    atts = gather_pieces(out_attention, tp)
    group = 2 if (rows // CHUNK) % 2 == 0 else 1
    out_local, turned, end = call(
        functools.partial(recurrent_body, group),
        [shape((rows, features), F32)] * 2 + [shape((pairs, 2 * HD, LANES), BF16)],
        (r, k, v, log_decay, learn_rate.reshape(1, -1)),
        [pltpu.VMEM((pairs, 2 * LANES, LANES), F32)],
        flops=2e10,
    )
    ends = [
        lax.ppermute(end, "sp", [(i, i + d) for i in range(sp - d)]) for d in range(sp - 1, 0, -1)
    ]
    far = [flip(block, "sp", sp, 1) for block in near]
    top, row_sum, acc = call(
        functools.partial(near_body, len(near)),
        [shape((heads, 2 * rows, 1), F32)] * 2 + [shape((heads, 2 * rows, LANES), F32)],
        (queries, *near),
        flops=1e10,
    )
    rec_mix = call(
        functools.partial(finish_body, len(ends)),
        [shape((rows, features), BF16)],
        (out_local, turned, *ends),
        flops=2e9,
    )[0]
    far_args = (queries, mix_lambda, *far, top, row_sum, acc)
    specs = vmem(len(far_args))
    specs[1] = pl.BlockSpec(memory_space=pltpu.SMEM)
    att_mix, log_sums = pl.pallas_call(
        functools.partial(far_body, len(far)),
        out_shape=[shape((rows, wide), BF16), shape((heads, 2, rows, 1), F32)],
        in_specs=specs,
        out_specs=vmem(2),
        compiler_params=pltpu.CompilerParams(vmem_limit_bytes=56 * 1024 * 1024),
        cost_estimate=pl.CostEstimate(
            flops=10_000_000_000, bytes_accessed=8_000_000, transcendentals=0
        ),
    )(*far_args)
    mix = jnp.concatenate([rec_mix, att_mix], axis=1).reshape(tp, rows // tp, features + wide)
    me = lax.axis_index("tp")
    moved = []
    for turn in range(tp):
        part = lax.dynamic_index_in_dim(mix, me ^ turn, 0, False)
        moved.append(part if turn == 0 else flip(part, "tp", tp, turn))
    layer_out = call(
        functools.partial(output_body, tp),
        [shape((rows // tp, out_recurrent.shape[1]), BF16)],
        (*moved, *recs, *atts, out_gain.reshape(1, -1)),
        flops=2e9,
    )[0]
    return (layer_out, log_sums.reshape(heads, 2, rows))


def solution(mesh):
    in_specs = (
        P("sp", "tp"),
        P(),
        P(None, "tp"),
        P(None, "tp"),
        P(None, "tp"),
        P(),
        P(None, "tp"),
        P("tp"),
        P("sp", "tp"),
        P("tp"),
        P(None, "tp", None),
        P(None, "tp", None),
        P(None, "tp", None),
        P("tp"),
        P("tp", None),
        P("tp", None),
        P(),
    )
    out_specs = (P(("sp", "tp"), None), P("tp", None, "sp"))
    body = functools.partial(per_device, mesh.shape["sp"], mesh.shape["tp"])
    return jax.shard_map(
        body, mesh=mesh, in_specs=in_specs, out_specs=out_specs, check_vma=False
    )
```

```python
import functools
import math

import jax
import jax.numpy as jnp
from jax import lax
from jax.experimental import pallas as pl
from jax.experimental.pallas import tpu as pltpu
from jax.sharding import PartitionSpec as P

HD = 64
LANES = 128
CHUNK = 64
DECAY_SCALE = math.exp(-0.5)
NORM_EPS = 1e-06
GROUP_EPS = 0.00064
HEAD_EPS = 1e-05
KEY_EPS = 1e-06
NEGATIVE = -1e30
F32 = jnp.float32
BF16 = jnp.bfloat16

NN = (((1,), (0,)), ((), ()))
NT = (((1,), (1,)), ((), ()))
TN = (((0,), (0,)), ((), ()))


def dot1(a, b, dims=NN):
    return lax.dot_general(a.astype(BF16), b.astype(BF16), dims, preferred_element_type=F32)


def halves(a):
    high = a.astype(BF16)
    return high, (a - high.astype(F32)).astype(BF16)


def dot3(a, b, dims=NN):
    ah, al = halves(a)
    bh, bl = halves(b)
    one = functools.partial(lax.dot_general, dimension_numbers=dims, preferred_element_type=F32)
    return one(ah, bh) + (one(al, bh) + one(ah, bl))


def swapped(place, turn):
    bit = 1
    while bit <= turn:
        if turn & bit:
            place = place + bit - 2 * bit * lax.rem(lax.div(place, bit), 2)
        bit *= 2
    return place


def normalize(pieces, gain, normed, me):
    count = len(pieces)
    width = pieces[0].shape[1]
    wides = [piece[...].astype(F32) for piece in pieces]
    total = sum(jnp.sum(wide * wide, axis=-1, keepdims=True) for wide in wides)
    scale = lax.rsqrt(total / (width * count) + NORM_EPS)
    for turn, wide in enumerate(wides):
        columns = pl.ds(pl.multiple_of(swapped(me, turn) * width, LANES), width)
        normed[:, columns] = (wide * scale * gain[:, columns]).astype(BF16)


def recurrent_body(group, r_ref, k_ref, v_ref, d_ref, learn_ref, out_ref, turn_ref, end_ref, state):
    rows, features = r_ref.shape
    pairs = features // LANES
    lane = lax.broadcasted_iota(jnp.int32, (1, LANES), 1)
    first = (lane < HD).astype(F32)
    second = 1.0 - first
    line = lax.broadcasted_iota(jnp.int32, (LANES, LANES), 0)
    column = lax.broadcasted_iota(jnp.int32, (LANES, LANES), 1)
    strict = line > column
    causal = line >= column
    eye = (line == column).astype(F32)
    same_head = ((line // HD) == (column // HD)).astype(BF16)
    small_line = lax.broadcasted_iota(jnp.int32, (CHUNK, CHUNK), 0)
    small_column = lax.broadcasted_iota(jnp.int32, (CHUNK, CHUNK), 1)
    lower = (small_line >= small_column).astype(BF16)

    def below(size):
        return ((line // size) == (column // size) + 1) & ((line // size) % 2 == 1)

    def spread(x):
        return jnp.concatenate([x * first, x * second], axis=0)

    for pair in range(pairs):
        state[pair, :LANES, :] = jnp.zeros((LANES, LANES), F32)
        state[pair, LANES:, :] = eye

    def local(pair, at):
        here = (pl.ds(at, CHUNK), pl.ds(pair * LANES, LANES))
        r = r_ref[here].astype(F32)
        k = k_ref[here].astype(F32)
        v = v_ref[here].astype(F32)
        decay = d_ref[here]
        learn = learn_ref[:, pl.ds(pair * LANES, LANES)]
        dh = decay.astype(BF16)
        rest = decay - dh.astype(F32)
        dm = rest.astype(BF16)
        dl = (rest - dm.astype(F32)).astype(BF16)
        running = dot1(lower, dh) + (dot1(lower, dm) + dot1(lower, dl))
        before = running - decay
        middle = running[CHUNK // 2 - 1 : CHUNK // 2, :]
        ending = running[CHUNK - 1 :, :]
        sh, sl = halves(k * k)
        squares = dot1(sh, same_head) + dot1(sl, same_head)
        unit = k * lax.rsqrt(squares + KEY_EPS)
        erase = unit * learn
        rise = jnp.exp(middle - running)
        left = jnp.concatenate(
            [spread(-unit * jnp.exp(before - middle)), spread(r * jnp.exp(running - middle))], axis=0
        )
        right = jnp.concatenate([spread(erase * rise), spread(k * rise)], axis=0)
        to_end = jnp.exp(ending - running)
        return dict(
            left=left,
            right=right,
            against=spread(-unit * jnp.exp(before)),
            read=spread(r * jnp.exp(running)),
            erase_end=spread(erase * to_end),
            keys_end=spread(k * to_end),
            values=spread(v),
            whole=jnp.exp(ending),
        )

    def step(turn, carry):
        spots = [(turn * group + g, pair) for g in range(group) for pair in range(pairs)]
        items = [local(pair, pl.multiple_of(c * CHUNK, CHUNK)) for c, pair in spots]
        for it in items:
            scores = dot3(it["left"], it["right"], NT)
            it["low"] = jnp.where(strict, scores[:LANES, :LANES], 0.0)
            it["carry"] = jnp.where(strict, scores[:LANES, LANES:], 0.0)
            it["read_erase"] = jnp.where(causal, scores[LANES:, :LANES], 0.0)
            it["read_keys"] = jnp.where(causal, scores[LANES:, LANES:], 0.0)
            it["inv"] = eye + jnp.where(below(1), it["low"], 0.0)
        size = 2
        while size < CHUNK:
            keep = below(size)
            for it in items:
                it["mid"] = dot3(jnp.where(keep, it["low"], 0.0), it["inv"])
            for it in items:
                it["inv"] = it["inv"] + dot3(it["inv"], it["mid"])
            size *= 2
        for it in items:
            it["fed"] = dot3(it["carry"], it["values"])
        for it in items:
            side = jnp.concatenate([it["against"], it["fed"]], axis=1)
            it["solved"] = dot3(it["inv"], side)
        for it in items:
            seen = dot1(it["read_erase"], it["solved"])
            it["heard"] = seen[:, LANES:] + dot1(it["read_keys"], it["values"])
            it["read"] = it["read"] + seen[:, :LANES]
            it["added"] = dot3(it["values"], it["keys_end"], TN)
        for (c, pair), it in zip(spots, items):
            now = state[pair]
            both = jnp.concatenate([it["solved"][:, :LANES], it["read"]], axis=0)
            met = dot3(both, now, NT)
            gone = jnp.concatenate(
                [met[:LANES, :LANES] + it["solved"][:, LANES:], met[:LANES, LANES:]], axis=1
            )
            later = now * it["whole"] + dot3(gone, it["erase_end"], TN)
            state[pair, :LANES, :] = later[:LANES] + it["added"]
            state[pair, LANES:, :] = later[LANES:]
            heard = met[LANES:, :LANES] + it["heard"]
            turned = met[LANES:, LANES:]
            here = (pl.ds(pl.multiple_of(c * CHUNK, CHUNK), CHUNK), pl.ds(pair * LANES, LANES))
            out_ref[here] = heard[:CHUNK] + heard[CHUNK:]
            turn_ref[here] = turned[:CHUNK] + turned[CHUNK:]
        return carry

    lax.fori_loop(0, rows // CHUNK // group, step, 0)
    for pair in range(pairs):
        now = state[pair]
        end_ref[pair, :HD, :] = (now[:HD] + now[HD:LANES]).astype(BF16)
        end_ref[pair, HD:, :] = (now[LANES : LANES + HD] + now[LANES + HD :]).astype(BF16)


def finish_body(out_ref, turn_ref, ends, place, mix_ref):
    pairs = out_ref.shape[1] // LANES
    lane = lax.broadcasted_iota(jnp.int32, (1, LANES), 1)
    first = (lane < HD).astype(F32)
    second = 1.0 - first
    line = lax.broadcasted_iota(jnp.int32, (LANES, LANES), 0)
    column = lax.broadcasted_iota(jnp.int32, (LANES, LANES), 1)
    same_head = ((line // HD) == (column // HD)).astype(BF16)

    def spread(x):
        return jnp.concatenate([x * first, x * second], axis=0)

    for pair in range(pairs):
        entering = jnp.zeros((LANES, LANES), F32)
        for far, end in ends:
            block = jnp.where(place >= far, end[pair].astype(F32), 0.0)
            high, low = halves(entering)
            move = spread(block[HD:])
            entering = dot1(high, move) + dot1(low, move) + spread(block[:HD])
        columns = pl.ds(pair * LANES, LANES)
        full = out_ref[:, columns] + dot3(turn_ref[:, columns], entering, NT)

        def mean(x):
            high, low = halves(x)
            return (dot1(high, same_head) + dot1(low, same_head)) * (1.0 / HD)

        centered = full - mean(full)
        mix_ref[:, columns] = (centered * lax.rsqrt(mean(centered * centered) + GROUP_EPS)).astype(
            BF16
        )


def attend(q, blocks, valid, heads, head, at, tile, diagonal, earlier):
    lane = lax.broadcasted_iota(jnp.int32, (1, LANES), 1)
    part = q[pl.ds(at, tile), pl.ds(head * LANES, LANES)].astype(F32) * HD ** (-0.5)
    both = jnp.concatenate(
        [jnp.where(lane < HD, part, 0.0), jnp.where(lane < HD, 0.0, part)], axis=0
    ).astype(BF16)
    scores = []
    for number, (block, fine) in enumerate(zip(blocks, valid)):
        s = lax.dot_general(
            both, block[:, pl.ds(head * LANES, LANES)], NT, preferred_element_type=F32
        )
        if number == 0 and diagonal:
            line = lax.broadcasted_iota(jnp.int32, (tile, s.shape[1]), 0) + at
            seen = line >= lax.broadcasted_iota(jnp.int32, (tile, s.shape[1]), 1)
            s = jnp.where(jnp.concatenate([seen, seen], axis=0), s, NEGATIVE)
        else:
            s = jnp.where(fine, s, NEGATIVE)
        scores.append(s)
    top = functools.reduce(jnp.maximum, [jnp.max(s, axis=-1, keepdims=True) for s in scores])
    if earlier is not None:
        top = jnp.maximum(top, earlier[0])
    row_sum, acc = 0.0, 0.0
    for s, block in zip(scores, blocks):
        weights = jnp.exp(s - top)
        row_sum = row_sum + jnp.sum(weights, axis=-1, keepdims=True)
        acc = acc + jnp.dot(
            weights.astype(BF16),
            block[:, pl.ds((heads + head) * LANES, LANES)],
            preferred_element_type=F32,
        )
    if earlier is not None:
        fade = jnp.exp(earlier[0] - top)
        row_sum = row_sum + earlier[1] * fade
        acc = acc + earlier[2] * fade
    return top, row_sum, acc


def tiles_of(rows):
    tile = LANES if rows % LANES == 0 else rows
    return tile, range(0, rows, tile)


def near_body(q, blocks, place, top_ref, sum_ref, acc_ref):
    count = len(blocks)
    rows, features = q.shape
    heads = features // LANES
    tile, starts = tiles_of(rows)
    valid = [place >= 2 * turn for turn in range(count)]
    for head in range(heads):
        for at in starts:
            top, row_sum, acc = attend(q, blocks, valid, heads, head, at, tile, True, None)
            here = pl.ds(2 * at, 2 * tile)
            top_ref[head, here, :] = top
            sum_ref[head, here, :] = row_sum
            acc_ref[head, here, :] = acc


def far_body(q, lam_ref, blocks, place, top_ref, sum_ref, acc_ref, mix_ref, shift, log_ref):
    count = len(blocks)
    rows, features = q.shape
    heads = features // LANES
    other = swapped(place, 1)
    tile, starts = tiles_of(rows)
    valid = [(other >= 2 * turn) & (other - 2 * turn < place) for turn in range(count)]
    for head in range(heads):
        lam = lam_ref[head]
        for at in starts:
            here = pl.ds(2 * at, 2 * tile)
            earlier = (top_ref[head, here, :], sum_ref[head, here, :], acc_ref[head, here, :])
            top, row_sum, acc = attend(q, blocks, valid, heads, head, at, tile, False, earlier)
            maps = acc / row_sum
            logs = top + jnp.log(row_sum)
            flat = jnp.transpose(jnp.broadcast_to(logs, (2 * tile, LANES)))
            log_ref[head, 0:1, pl.ds(at, tile)] = flat[:1, :tile]
            log_ref[head, 1:2, pl.ds(at, tile)] = flat[:1, tile:]
            out = maps[:tile] - lam * maps[tile:]
            out = out * lax.rsqrt(jnp.mean(out * out, axis=-1, keepdims=True) + HEAD_EPS)
            mix_ref[pl.ds(at, tile), pl.ds(shift + head * LANES, LANES)] = out.astype(BF16)


def layer_body(sp, tp, *refs):
    (hidden, gain, wr_h, wk_h, wv_h, down_h, up_h, base, shift, learn) = refs[:10]
    (wq_h, wkp_h, wvp_h, lam, rec_h, att_h, out_gain, out, logs) = refs[10:19]
    (xs, normed, wr, wk, wv, down, up, wq, wkp, wvp, hw) = refs[19:30]
    (near, far, r, k, v, d, q, heard, turned, ends, state) = refs[30:41]
    (top, row_sum, acc, mix, moved) = refs[41:46]
    (load, x_send, x_recv, w_send, w_recv, n_send, n_recv) = refs[46:53]
    (f_send, f_recv, e_send, e_recv, m_send, m_recv) = refs[53:]
    rows, features = r.shape
    wide = q.shape[1]
    me = lax.axis_index("tp")
    place = lax.axis_index("sp")
    count = sp // 2

    barrier = pltpu.get_barrier_semaphore()
    for turn in range(1, tp):
        pl.semaphore_signal(barrier, inc=1, device_id={"tp": swapped(me, turn)})
    for hop in range(1, sp):
        pl.semaphore_signal(barrier, inc=1, device_id={"sp": lax.rem(place + hop, sp)})
    loads = []
    for number, (source, target) in enumerate(
        (
            (wkp_h, wkp),
            (wvp_h, wvp),
            (wq_h, wq),
            (wr_h, wr),
            (wk_h, wk),
            (wv_h, wv),
            (down_h, down),
            (up_h, up),
            (rec_h, hw.at[0, pl.ds(0, features)]),
            (att_h, hw.at[0, pl.ds(features, wide)]),
        )
    ):
        loads.append(pltpu.make_async_copy(source, target, load.at[number]))
        loads[-1].start()
    pl.semaphore_wait(barrier, tp - 1 + sp - 1)

    def remote(source, target, send, recv, slot, device):
        return pltpu.make_async_remote_copy(
            src_ref=source,
            dst_ref=target,
            send_sem=send.at[slot],
            recv_sem=recv.at[slot],
            device_id=device,
        )

    def spreading(own, slots, send, recv):
        def source(turn):
            return own if turn == 0 else slots.at[turn]

        copies = {}
        for turn in range(1, tp):
            if turn % 2 == 0:
                copies[turn] = remote(
                    own, slots.at[turn], send, recv, turn, {"tp": swapped(me, turn)}
                )
            else:
                copies[turn] = remote(
                    source(turn - 1), slots.at[turn], send, recv, turn, {"tp": swapped(me, 1)}
                )
        return copies

    hops = spreading(hidden, xs, x_send, x_recv)
    for turn in range(2, tp, 2):
        hops[turn].start()
    hops[1].start()
    for turn in range(2, tp, 2):
        hops[turn].wait_recv()
        hops[turn + 1].start()
    for turn in range(1, tp, 2):
        hops[turn].wait_recv()
    loads[8].wait()
    loads[9].wait()
    outs = spreading(hw.at[0], hw, w_send, w_recv)
    for turn in range(2, tp, 2):
        outs[turn].start()
    outs[1].start()
    normalize([hidden] + [xs.at[turn] for turn in range(1, tp)], gain, normed, me)

    def product(weight):
        return jnp.dot(normed[...], weight[...], preferred_element_type=F32)

    for one in loads[:8]:
        one.wait()
    near[0, :, :wide] = product(wkp).astype(BF16)
    near[0, :, wide:] = product(wvp).astype(BF16)
    q[...] = product(wq).astype(BF16)
    nears = {
        turn: remote(
            near.at[0],
            near.at[turn],
            n_send,
            n_recv,
            turn,
            {"sp": lax.rem(place + 2 * turn, sp)},
        )
        for turn in range(1, count)
    }
    fars = [
        remote(near.at[turn], far.at[turn], f_send, f_recv, turn, {"sp": swapped(place, 1)})
        for turn in range(count)
    ]
    for turn in range(1, count):
        nears[turn].start()
    fars[0].start()
    r[...] = product(wr).astype(BF16)
    k[...] = product(wk).astype(BF16)
    v[...] = product(wv).astype(BF16)
    low_rank = jnp.tanh(product(down)).astype(BF16)
    pre = jnp.dot(low_rank, up[...], preferred_element_type=F32) + base[...]
    d[...] = -DECAY_SCALE * jax.nn.sigmoid(pre) + shift[...]

    group = 2 if (rows // CHUNK) % 2 == 0 else 1
    recurrent_body(group, r, k, v, d, learn, heard, turned, ends.at[0], state)
    states = {
        hop: remote(
            ends.at[0], ends.at[hop], e_send, e_recv, hop, {"sp": lax.rem(place + hop, sp)}
        )
        for hop in range(1, sp)
    }
    for hop in range(1, sp):
        states[hop].start()
    for turn in range(1, count):
        nears[turn].wait_recv()
        fars[turn].start()
    near_body(q, [near.at[turn] for turn in range(count)], place, top, row_sum, acc)
    for hop in range(1, sp):
        states[hop].wait_recv()
    finish_body(
        heard, turned, [(hop, ends.at[hop]) for hop in range(sp - 1, 0, -1)], place, mix
    )
    for turn in range(2, tp, 2):
        outs[turn].wait_recv()
        outs[turn + 1].start()
    for turn in range(count):
        fars[turn].wait_recv()
    far_body(
        q,
        lam,
        [far.at[turn] for turn in range(count)],
        place,
        top,
        row_sum,
        acc,
        mix,
        features,
        logs,
    )
    part = rows // tp
    mixes = {}
    for turn in range(1, tp):
        owner = swapped(me, turn)
        mixes[turn] = remote(
            mix.at[pl.ds(pl.multiple_of(owner * part, part), part)],
            moved.at[turn],
            m_send,
            m_recv,
            turn,
            {"tp": owner},
        )
    for turn in list(range(2, tp)) + [1]:
        mixes[turn].start()
    total = jnp.dot(
        mix[pl.ds(pl.multiple_of(me * part, part), part), :], hw[0], preferred_element_type=F32
    )
    for turn in range(1, tp):
        mixes[turn].wait_recv()
        if turn % 2:
            outs[turn].wait_recv()
        total = total + jnp.dot(moved[turn], hw[turn], preferred_element_type=F32)
    mean = jnp.mean(total * total, axis=-1, keepdims=True)
    out[...] = (total * lax.rsqrt(mean + NORM_EPS) * out_gain[...]).astype(BF16)
    for group_of in (hops, outs, nears, states, mixes):
        for one in group_of.values():
            one.wait_send()
    for one in fars:
        one.wait_send()


def per_device(
    sp,
    tp,
    hidden_in,
    in_gain,
    receptance_weight,
    key_weight,
    value_weight,
    decay_down,
    decay_up,
    decay_base,
    decay_shift,
    learn_rate,
    query_pair,
    key_pair,
    value_pair,
    mix_lambda,
    out_recurrent,
    out_attention,
    out_gain,
):
    rows, width = hidden_in.shape
    depth = width * tp
    features = receptance_weight.shape[1]
    heads = mix_lambda.shape[0]
    wide = heads * LANES
    pairs = features // LANES
    low = decay_down.shape[1]
    across = out_recurrent.shape[1]
    part = rows // tp
    count = sp // 2
    shape = jax.ShapeDtypeStruct
    held = pltpu.VMEM
    args = (
        hidden_in,
        in_gain.reshape(1, -1),
        receptance_weight,
        key_weight,
        value_weight,
        decay_down,
        decay_up,
        decay_base.reshape(1, -1),
        decay_shift,
        learn_rate.reshape(1, -1),
        query_pair.reshape(depth, wide),
        key_pair.reshape(depth, wide),
        value_pair.reshape(depth, wide),
        mix_lambda,
        out_recurrent,
        out_attention,
        out_gain.reshape(1, -1),
    )
    inside = pl.BlockSpec(memory_space=pltpu.VMEM)
    outside = pl.BlockSpec(memory_space=pl.ANY)
    specs = [inside] * 2 + [outside] * 5 + [inside] * 3 + [outside] * 3
    specs += [pl.BlockSpec(memory_space=pltpu.SMEM)] + [outside] * 2 + [inside]
    sizes = (10, tp, tp, tp, tp, count, count, count, count, sp, sp, tp, tp)
    return tuple(
        pl.pallas_call(
            functools.partial(layer_body, sp, tp),
            out_shape=[shape((part, across), BF16), shape((heads, 2, rows), F32)],
            in_specs=specs,
            out_specs=[inside] * 2,
            scratch_shapes=[
                held((tp, rows, width), BF16),
                held((rows, depth), BF16),
                held((depth, features), BF16),
                held((depth, features), BF16),
                held((depth, features), BF16),
                held((depth, low), BF16),
                held((low, features), BF16),
                held((depth, wide), BF16),
                held((depth, wide), BF16),
                held((depth, wide), BF16),
                held((tp, features + wide, across), BF16),
                held((count, rows, 2 * wide), BF16),
                held((count, rows, 2 * wide), BF16),
                held((rows, features), BF16),
                held((rows, features), BF16),
                held((rows, features), BF16),
                held((rows, features), F32),
                held((rows, wide), BF16),
                held((rows, features), F32),
                held((rows, features), F32),
                held((sp, pairs, 2 * HD, LANES), BF16),
                held((pairs, 2 * LANES, LANES), F32),
                held((heads, 2 * rows, 1), F32),
                held((heads, 2 * rows, 1), F32),
                held((heads, 2 * rows, LANES), F32),
                held((rows, features + wide), BF16),
                held((tp, part, features + wide), BF16),
            ]
            + [pltpu.SemaphoreType.DMA((size,)) for size in sizes],
            compiler_params=pltpu.CompilerParams(
                collective_id=0, has_side_effects=True, vmem_limit_bytes=62 * 1024 * 1024
            ),
        )(*args)
    )


def solution(mesh):
    in_specs = (
        P("sp", "tp"),
        P(),
        P(None, "tp"),
        P(None, "tp"),
        P(None, "tp"),
        P(),
        P(None, "tp"),
        P("tp"),
        P("sp", "tp"),
        P("tp"),
        P(None, "tp", None),
        P(None, "tp", None),
        P(None, "tp", None),
        P("tp"),
        P("tp", None),
        P("tp", None),
        P(),
    )
    out_specs = (P(("sp", "tp"), None), P("tp", None, "sp"))
    body = functools.partial(per_device, mesh.shape["sp"], mesh.shape["tp"])
    return jax.shard_map(
        body, mesh=mesh, in_specs=in_specs, out_specs=out_specs, check_vma=False
    )
```
